32 devices in a mesh: ep: 4 (over y, x), tp: 8 (over z, core).
Axes of the slice: x: 2, y: 2, z: 4, core: 2. Of those that a mesh axis runs over, the one named last changes fastest.
Arguments:
- tokens: bfloat16 [256, 4096], P(('ep', 'tp')), may hold values from -6 to 6
- rec_state: float32 [256, 2048], P('ep', 'tp'), may hold values from -40 to 40
- conv_state: bfloat16 [256, 3, 2048], P('ep', None, 'tp'), may hold values from -6 to 6
- route_ids: int32 [256, 4], P('ep'), may hold values from 0 to 15, all different within a row; in each aligned block of 8 rows (0 to 7, 8 to 15, ...) at most 2 rows name the same one
- route_weights: float32 [256, 4], P(('ep', 'tp')), may hold values from 0.1 to 1
- first_gain: bfloat16 [4096], replicated, may hold values from 0.099609375 to 1.8984375
- proj_input: bfloat16 [4096, 2048], P(None, 'tp'), may hold values from -0.09375 to 0.09375
- proj_gate: bfloat16 [4096, 2048], P(None, 'tp'), may hold values from -0.09375 to 0.09375
- conv_taps: bfloat16 [4, 2048], replicated, may hold values from -1.5 to 1.5
- decay_logit: float32 [2048], replicated, may hold values from 1 to 6
- block_decay: bfloat16 [16, 128, 128], replicated, may hold values from -0.5 to 0.5
- block_input: bfloat16 [16, 128, 128], replicated, may hold values from -0.5 to 0.5
- rec_gain: bfloat16 [2048], replicated, may hold values from 0.099609375 to 1.8984375
- proj_out: bfloat16 [2048, 4096], P('tp'), may hold values from -0.125 to 0.125
- second_gain: bfloat16 [4096], replicated, may hold values from 0.099609375 to 1.8984375
- expert_gate: bfloat16 [16, 4096, 4096], P('ep', None, 'tp'), may hold values from -0.21875 to 0.21875
- expert_up: bfloat16 [16, 4096, 4096], P('ep', None, 'tp'), may hold values from -0.21875 to 0.21875
- expert_down: bfloat16 [16, 4096, 4096], P('ep', 'tp'), may hold values from -0.0234375 to 0.0234375
Outputs:
- result: bfloat16 [256, 4096], P(('ep', 'tp'))
- new_state: float32 [256, 2048], P('ep', 'tp')
- new_conv: bfloat16 [256, 3, 2048], P('ep', None, 'tp')
The draws below stay inside these ranges and needn't reach their ends.
Inputs may be any that keep to these rules, and one draw needn't show every extreme that they name: `route_ids`: each row names 4 different experts; in the rows of one device (aligned blocks of 8 rows) no expert is named by more than 2 rows, and one is named by exactly 2.
All inputs are finite; a program needn't handle non-finite values.
Results may differ from the reference program's by a relative error of at most 0.025.
Values may be sent and summed in bfloat16 or wider, within the bound.
No kernel may reach another device: no remote copies, remote signals or barrier semaphores. Data moves between devices by JAX's collectives and lax.ppermute only.
A program may use at most 128 MiB of HBM per device.

```python
import math
import jax
import jax.numpy as jnp
import numpy as np
from jax import lax

D = 4096
D_REC = 2048
REC_BLOCKS = 16
BLOCK_W = 128
TAPS = 4
FF = 4096
EXPERTS = 16
TOP_K = 4
TOK = 8
CAP = 2
BATCH = 256
N_EP = 4
N_TP = 8


def draw_rec_state(key, part):
    key_base, key_rows = jax.random.split(jax.random.fold_in(key, 11), 2)
    column = jnp.arange(D_REC, dtype=jnp.float32) / D_REC
    column_scale = 0.4 * jnp.exp(column * math.log(8.0))
    row_scale = jnp.exp(jax.random.uniform(key_rows, (BATCH, 1), jnp.float32, math.log(0.3), math.log(3.0)))
    base = jnp.clip(jax.random.normal(key_base, (BATCH, D_REC), jnp.float32), -4.0, 4.0)
    return base * row_scale * column_scale


def steps_of(stream_key, shape, cuts, least, top_value):
    level, own = 1.0, jax.random.fold_in(stream_key, 6)
    for dim, shards_of in cuts:
        draws = jnp.exp(jax.random.uniform(jax.random.fold_in(own, dim), (shards_of,), jnp.float32, least / len(cuts), top_value / len(cuts)))
        level = level * jnp.repeat(draws, shape[dim] // shards_of).reshape([-1 if axis == dim else 1 for axis in range(len(shape))])
    return level


def routed_block(own_key, own, number, rows, number_of, top, most, lean):
    order = jax.random.permutation(own_key, number_of)
    packed, common = shares(number_of, rows * top, most, lean, True), shares(number_of, rows * top, most, lean, False)
    places = jnp.arange(number_of)

    def named(lengths, turn):
        used = int((lengths > 0).sum())
        fixed = max(1, used // 4)
        passed = fixed + (places - fixed + turn * (used - fixed)) % max(1, number_of - fixed)
        return jnp.zeros((number_of,), jnp.int32).at[order[jnp.where(places < fixed, places, passed)]].set(jnp.asarray(lengths, jnp.int32))

    lengths = jnp.where(number % 4 == 0, named(packed, number // 4), named(common, number - number // 4 - 1))
    mixed = jax.random.permutation(jax.random.fold_in(own, 3), number_of)
    donor, receiver = mixed[0:number_of // 2 * 2:2], mixed[1:number_of // 2 * 2:2]
    room = jnp.minimum(lengths[donor] - 1, most - lengths[receiver]) // 2
    room = jnp.where((donor == order[0]) | (receiver == order[0]) | (lengths[receiver] == 0), 0, jnp.maximum(room, 0))
    passed = jax.random.randint(jax.random.fold_in(own, 4), (number_of // 2,), 0, 1 << 20) % (room + 1)
    lengths = lengths.at[donor].add(-passed).at[receiver].add(passed)
    labels = jnp.searchsorted(jnp.cumsum(lengths), jnp.arange(rows * top), side="right").astype(jnp.int32)
    table = labels.reshape(top, rows).T
    table = table[jax.random.permutation(jax.random.fold_in(own, 1), rows)]
    turn = jax.random.randint(jax.random.fold_in(own, 2), (rows, 1), 0, top)
    return jnp.take_along_axis(table, (jnp.arange(top)[None, :] + turn) % top, axis=1)


def shares(count, total, limit, slope, full):
    loads = [(1 << 20) // math.isqrt(grade ** slope) + 1 for grade in range(1, count + 1)]
    largest = limit if full else min(limit, max(-(-total // count), total * loads[0] // sum(loads)))
    least = 1 if total - largest >= count - 1 else 0
    counts, rest = [largest] + [least] * (count - 1), total - largest - least * (count - 1)
    while rest > 0:
        movable = [i for i in range(1, count) if counts[i] < largest] or [i for i in range(1, count) if counts[i] < limit]
        pool, remaining = sum([loads[i] for i in movable]), rest
        for i in movable:
            extra = min(limit - counts[i], max(1, remaining * loads[i] // pool), rest)
            counts[i] = counts[i] + extra
            rest = rest - extra
    return np.array(counts)


def centred(own_key, extent, width, most, cuts=(), held_as=jnp.bfloat16):
    loudness = steps_of(own_key, extent, cuts, -0.22, 0.18) if cuts else 1.0
    entries = jax.random.normal(own_key, extent, jnp.float32) * width * loudness
    return jnp.minimum(jnp.maximum(entries, -most), most).astype(held_as)


def setup_inputs(seed: int = 0) -> dict:
    seeds = jax.random.split(jax.random.key(seed), 19)
    tokens = centred(seeds[0], (BATCH, D), 1.0, 6.0, ((0, 32),))
    rec_state = draw_rec_state(jax.random.fold_in(seeds[18], 71), 0)
    conv_state = centred(seeds[2], (BATCH, TAPS - 1, D_REC), 1.0, 6.0, ((0, 4), (2, 8)))
    route_ids_keys = jax.random.split(jax.random.fold_in(seeds[3], 1), BATCH // TOK)
    route_ids_turns = jax.random.permutation(jax.random.fold_in(seeds[3], 3), BATCH // TOK)
    route_ids = jax.vmap(lambda own, number: routed_block(jax.random.fold_in(seeds[3], 2), own, number, TOK, EXPERTS, TOP_K, CAP, 1))(route_ids_keys, route_ids_turns).reshape((BATCH, TOP_K))
    route_weights = jnp.clip(jnp.exp(math.log(1.0) - 2.3025851 * jax.random.uniform(seeds[4], (BATCH, TOP_K), jnp.float32) ** steps_of(seeds[4], (BATCH, TOP_K), ((0, 32),), -0.2, 0.2)), 0.1, 1.0)
    first_gain = jnp.clip(1.0 + 0.18 * jax.random.normal(seeds[5], (D,), jnp.float32), 0.099609375, 1.8984375).astype(jnp.bfloat16)
    proj_input = centred(seeds[6], (D, D_REC), D ** -0.5, 0.09375, ((1, 8),))
    proj_gate = centred(seeds[7], (D, D_REC), D ** -0.5, 0.09375, ((1, 8),))
    conv_taps = centred(seeds[8], (TAPS, D_REC), 0.25, 1.5)
    decay_logit = jnp.clip(jax.random.uniform(seeds[9], (D_REC,), jnp.float32, 1.0, 6.0), 1.0, 6.0)
    block_decay = centred(seeds[10], (REC_BLOCKS, BLOCK_W, BLOCK_W), BLOCK_W ** -0.5, 0.5)
    block_input = centred(seeds[11], (REC_BLOCKS, BLOCK_W, BLOCK_W), BLOCK_W ** -0.5, 0.5)
    rec_gain = jnp.clip(1.0 + 0.18 * jax.random.normal(seeds[12], (D_REC,), jnp.float32), 0.099609375, 1.8984375).astype(jnp.bfloat16)
    proj_out = centred(seeds[13], (D_REC, D), D_REC ** -0.5, 0.125, ((0, 8),))
    second_gain = jnp.clip(1.0 + 0.18 * jax.random.normal(seeds[14], (D,), jnp.float32), 0.099609375, 1.8984375).astype(jnp.bfloat16)
    expert_gate = centred(seeds[15], (EXPERTS, D, FF), (D // 6) ** -0.5, 0.21875, ((0, 4), (2, 8)))
    expert_up = centred(seeds[16], (EXPERTS, D, FF), (D // 6) ** -0.5, 0.21875, ((0, 4), (2, 8)))
    expert_down = centred(seeds[17], (EXPERTS, FF, D), (FF * 16) ** -0.5, 0.0234375, ((0, 4), (1, 8)))
    return dict(tokens=tokens, rec_state=rec_state, conv_state=conv_state, route_ids=route_ids, route_weights=route_weights, first_gain=first_gain, proj_input=proj_input, proj_gate=proj_gate, conv_taps=conv_taps, decay_logit=decay_logit, block_decay=block_decay, block_input=block_input, rec_gain=rec_gain, proj_out=proj_out, second_gain=second_gain, expert_gate=expert_gate, expert_up=expert_up, expert_down=expert_down)


EPS = 1e-06
CLAMP = 7.0
ALPHA = 1.702
RATE = 8.0

def norm_rows(values, gain):
    scale = lax.rsqrt(lax.optimization_barrier(jnp.mean(values * values, axis=-1, keepdims=True)) + EPS)
    return values * scale * gain.astype(jnp.float32)

def slot_positions(ids, blocks):
    rows, picks = ids.shape
    onehot = (ids[:, :, None] == jnp.arange(EXPERTS, dtype=jnp.int32)).astype(jnp.int32)
    onehot = onehot.reshape(blocks, rows // blocks * picks, EXPERTS)
    before = jnp.cumsum(onehot, axis=1) - onehot
    return lax.optimization_barrier(jnp.sum(before * onehot, axis=-1)).reshape(rows, picks).astype(jnp.int32)

def reference(tokens, rec_state, conv_state, route_ids, route_weights, first_gain, proj_input, proj_gate, conv_taps, decay_logit, block_decay, block_input, rec_gain, proj_out, second_gain, expert_gate, expert_up, expert_down):
    token_values = tokens.astype(jnp.float32)
    normed = norm_rows(token_values, first_gain).astype(jnp.bfloat16)
    branch_in = jnp.dot(normed, proj_input, preferred_element_type=jnp.float32).astype(jnp.bfloat16)
    branch_gate = jnp.dot(normed, proj_gate, preferred_element_type=jnp.float32).astype(jnp.bfloat16)
    tap_weights = conv_taps.astype(jnp.float32)
    conv_values = conv_state.astype(jnp.float32)
    conv_out = tap_weights[TAPS - 1] * branch_in.astype(jnp.float32)
    for tap in range(TAPS - 1):
        conv_out = conv_out + tap_weights[tap] * conv_values[:, tap]
    new_conv = jnp.concatenate([conv_state[:, 1:], branch_in[:, None, :]], axis=1)
    conv_low = lax.optimization_barrier(conv_out.astype(jnp.bfloat16)).astype(jnp.float32)
    blocked = conv_low.reshape(BATCH, REC_BLOCKS, BLOCK_W)
    decay_gate = jax.nn.sigmoid(jnp.einsum('rnk,nkj->rnj', blocked, block_decay.astype(jnp.float32)).reshape(BATCH, D_REC))
    input_gate = jax.nn.sigmoid(jnp.einsum('rnk,nkj->rnj', blocked, block_input.astype(jnp.float32)).reshape(BATCH, D_REC))
    log_keep = -RATE * decay_gate * jax.nn.softplus(-decay_logit)
    keep_factor = jnp.exp(log_keep)
    new_state = keep_factor * rec_state + jnp.sqrt(-jnp.expm1(2.0 * log_keep)) * input_gate * conv_out
    hidden = new_state * jax.nn.gelu(branch_gate.astype(jnp.float32))
    squares = lax.optimization_barrier(jnp.sum(hidden * hidden, axis=-1, keepdims=True))
    gained = (hidden * rec_gain.astype(jnp.float32)).astype(jnp.bfloat16)
    partial_value = jnp.dot(gained, proj_out, preferred_element_type=jnp.float32)
    residual = token_values + partial_value * lax.rsqrt(squares / D_REC + EPS)
    second = norm_rows(residual, second_gain).astype(jnp.bfloat16)
    devices = N_EP * N_TP
    tok_rows = BATCH // devices
    positions = slot_positions(route_ids, devices)
    row_owner = (jnp.arange(BATCH, dtype=jnp.int32) // tok_rows)[:, None]
    slots = row_owner * CAP + positions
    slot_count = devices * CAP
    row_index = jnp.broadcast_to(jnp.arange(BATCH, dtype=jnp.int32)[:, None], route_ids.shape)
    table = jnp.zeros((EXPERTS, slot_count), jnp.int32).at[route_ids, slots].set(row_index)

    def run_expert(expert):
        rows_in = second[table[expert]]
        gate = jnp.dot(rows_in, expert_gate[expert], preferred_element_type=jnp.float32)
        upper = jnp.dot(rows_in, expert_up[expert], preferred_element_type=jnp.float32)
        clipped = jnp.minimum(gate, CLAMP)
        act = ((jnp.clip(upper, -CLAMP, CLAMP) + 1.0) * (clipped * jax.nn.sigmoid(ALPHA * clipped))).astype(jnp.bfloat16)
        pieces = jnp.einsum('rtf,tfd->rtd', act.reshape(slot_count, N_TP, FF // N_TP).astype(jnp.float32), expert_down[expert].reshape(N_TP, FF // N_TP, D).astype(jnp.float32))
        rounded = lax.optimization_barrier(pieces.astype(jnp.bfloat16)).astype(jnp.float32)
        return lax.optimization_barrier(jnp.sum(rounded, axis=1)).astype(jnp.bfloat16)
    outputs = lax.map(run_expert, jnp.arange(EXPERTS, dtype=jnp.int32))
    picked = outputs[route_ids, slots].astype(jnp.float32)
    expert_mix = lax.optimization_barrier(jnp.sum(route_weights[:, :, None] * picked, axis=1))
    result = (residual + expert_mix).astype(jnp.bfloat16)
    return (result, new_state, new_conv)
```

```python
import functools

import jax
import jax.numpy as jnp
from jax import lax
from jax.experimental import pallas as pl
from jax.experimental.pallas import tpu as pltpu
from jax.sharding import PartitionSpec as P

EPS = 1e-06
CLAMP = 7.0
ALPHA = 1.702
RATE = 8.0
LANES = 128
F32 = jnp.float32
BF16 = jnp.bfloat16


VM = pl.BlockSpec(memory_space=pltpu.VMEM)
SM = pl.BlockSpec(memory_space=pltpu.SMEM)


def call(body, outs, args, limit_mib, name, smem=0, flops=10**8):
    specs = [SM] * smem + [VM] * (len(args) - smem)
    shapes = [jax.ShapeDtypeStruct(s, d) for s, d in outs]
    return pl.pallas_call(
        body,
        out_shape=shapes,
        in_specs=specs,
        out_specs=[VM] * len(outs),
        name=name,
        compiler_params=pltpu.CompilerParams(vmem_limit_bytes=limit_mib << 20),
        cost_estimate=pl.CostEstimate(flops=flops, bytes_accessed=10**6, transcendentals=0),
    )(*args)


def log2(n):
    return n.bit_length() - 1


def split_sum(values):
    high = values.astype(BF16)
    low = (values - high.astype(F32)).astype(BF16)
    lane = lax.broadcasted_iota(jnp.int32, values.shape, 1)
    return jnp.where(lane == 0, high.astype(F32), jnp.where(lane == 1, low.astype(F32), 0.0))


def minus_expm1(u):
    series = -u * (1.0 + u * (0.5 + u * (1.0 / 6.0 + u * (1.0 / 24.0 + u * (1.0 / 120.0)))))
    return jnp.where(u > -0.125, series, 1.0 - jnp.exp(u))


def recur_body(z_count, *refs):
    place_ref = refs[0]
    blocks = refs[1 : 1 + 2 * z_count]
    (gain_ref, win_ref, wgate_ref, convp_ref, tap_ref, dmat_ref, imat_ref, rate_ref, state_ref,
     rgain_ref, wout_ref) = refs[1 + 2 * z_count : 12 + 2 * z_count]
    newstate_ref, branch_ref, keep_ref, send_ref = refs[12 + 2 * z_count :]
    rows_each, width = blocks[0].shape
    rows = 2 * z_count * rows_each
    lw = win_ref.shape[1]
    gain = gain_ref[...].astype(F32)
    parts = []
    for b in blocks:
        v = b[...].astype(F32)
        scale = lax.rsqrt(jnp.mean(v * v, axis=-1, keepdims=True) + EPS)
        parts.append(v * scale * gain)
    normed = jnp.concatenate(parts, axis=0).astype(BF16)
    bin_rel = jnp.dot(normed, win_ref[...], preferred_element_type=F32).astype(BF16)
    bgate_rel = jnp.dot(normed, wgate_ref[...], preferred_element_type=F32).astype(BF16)
    place = place_ref[0]
    z_place = lax.shift_right_logical(place, 1)
    core = place & 1
    row = lax.broadcasted_iota(jnp.int32, (rows, rows), 0)
    col = lax.broadcasted_iota(jnp.int32, (rows, rows), 1)
    sh = log2(rows_each)
    blk = lax.shift_right_logical(col, sh)
    kk = blk & (z_count - 1)
    hh = lax.shift_right_logical(blk, log2(z_count))
    target = ((z_place ^ kk) * 2 + (core ^ hh)) * rows_each + (col & (rows_each - 1))
    order = jnp.where(row == target, 1.0, 0.0).astype(BF16)
    branch = jnp.dot(order, bin_rel, preferred_element_type=F32)
    bgate = jnp.dot(order, bgate_rel, preferred_element_type=F32)
    branch_ref[...] = branch.astype(BF16)
    conv = convp_ref[...] + tap_ref[...] * branch
    low = conv.astype(BF16)
    nb, bw = dmat_ref.shape[0], dmat_ref.shape[1]
    dec = jnp.concatenate(
        [jnp.dot(low[:, n * bw : (n + 1) * bw], dmat_ref[n], preferred_element_type=F32) for n in range(nb)], axis=1)
    inp = jnp.concatenate(
        [jnp.dot(low[:, n * bw : (n + 1) * bw], imat_ref[n], preferred_element_type=F32) for n in range(nb)], axis=1)
    log_keep = jax.nn.sigmoid(dec) * rate_ref[...]
    new_state = jnp.exp(log_keep) * state_ref[...] + jnp.sqrt(minus_expm1(2.0 * log_keep)) * jax.nn.sigmoid(inp) * conv
    newstate_ref[...] = new_state
    hidden = new_state * jax.nn.gelu(bgate)
    squares = jnp.sum(hidden * hidden, axis=1, keepdims=True)
    sq = split_sum(jnp.broadcast_to(squares, (rows, LANES))).astype(BF16)
    gained = (hidden * rgain_ref[...]).astype(BF16)
    back = (((0,), (0,)), ((), ()))
    g_rel = lax.dot_general(order, gained, back, preferred_element_type=F32).astype(BF16)
    s_rel = lax.dot_general(order, sq, back, preferred_element_type=F32)
    half = rows // 2
    mixed = jnp.dot(g_rel, wout_ref[...], preferred_element_type=F32)
    keep_ref[:, :width] = mixed[:half]
    keep_ref[:, width:] = s_rel[:half]
    send_ref[:, :width] = mixed[half:].astype(BF16)
    send_ref[:, width:] = s_rel[half:].astype(BF16)


def mix_body(z_count, keep_ref, recv_ref, *outs):
    rows_each, ext = outs[0].shape
    width = ext - LANES
    total = keep_ref[:, :width] + recv_ref[:, :width].astype(F32)
    tail = keep_ref[:, width:] + recv_ref[:, width:].astype(F32)
    squares = tail[:, 0:1] + tail[:, 1:2]
    sq = split_sum(jnp.broadcast_to(squares, tail.shape))
    for k in range(z_count):
        part = slice(k * rows_each, (k + 1) * rows_each)
        outs[k][:, :width] = total[part].astype(outs[k].dtype)
        outs[k][:, width:] = sq[part].astype(outs[k].dtype)


def second_body(channels, count, tok_ref, gain_ref, wdense_ref, *refs):
    parts, (res_ref, sec_ref) = refs[:count], refs[count:]
    width = tok_ref.shape[1]
    total = parts[0][:, :width].astype(F32)
    tail = parts[0][:, width:].astype(F32)
    for p in parts[1:]:
        total = total + p[:, :width].astype(F32)
        tail = tail + p[:, width:].astype(F32)
    squares = tail[:, 0:1] + tail[:, 1:2]
    residual = tok_ref[...].astype(F32) + total * lax.rsqrt(squares / channels + EPS)
    res_ref[...] = residual
    scale = lax.rsqrt(jnp.mean(residual * residual, axis=-1, keepdims=True) + EPS)
    sec_ref[:, :width] = (residual * scale * gain_ref[...].astype(F32)).astype(BF16)
    sec_ref[:, width:] = wdense_ref[...]


def cat_body(*refs):
    out = refs[-1]
    at = 0
    for r in refs[:-1]:
        out[at : at + r.shape[0]] = r[...]
        at += r.shape[0]


def gateup_body(count, rows_each, capacity, place_ref, *refs):
    pieces = refs[:count]
    gate_ref, up_ref, act_ref, comb_ref, x_ref, xs_ref = refs[count:]
    e_local, width, hid = gate_ref.shape
    each = pieces[0].shape[0]
    rows = count * each
    for i, p in enumerate(pieces):
        x_ref[i * each : (i + 1) * each, :] = p[...]
    weights = x_ref[:, width:].astype(F32)
    lane = lax.broadcasted_iota(jnp.int32, (LANES, LANES), 0)
    col = lax.broadcasted_iota(jnp.int32, (LANES, LANES), 1)
    pick = jnp.where((lane == col + place_ref[0] * e_local) & (col < e_local), 1.0, 0.0).astype(BF16)
    local = jnp.dot(x_ref[:, width:], pick, preferred_element_type=F32)
    mask = (local != 0.0).astype(F32)
    r0 = lax.broadcasted_iota(jnp.int32, (rows, rows), 0)
    c0 = lax.broadcasted_iota(jnp.int32, (rows, rows), 1)
    sh = log2(rows_each)
    same = lax.shift_right_logical(r0, sh) == lax.shift_right_logical(c0, sh)
    before = jnp.where(same & (c0 < r0), 1.0, 0.0).astype(BF16)
    rank = jnp.dot(before, mask.astype(BF16), preferred_element_type=F32)
    slots = rows // rows_each * capacity
    tok_blk = lax.shift_right_logical(lax.broadcasted_iota(jnp.int32, (rows, 1), 0), sh)
    slot_ids = lax.broadcasted_iota(jnp.int32, (rows, slots), 1)
    back = (((0,), (0,)), ((), ()))
    for e in range(e_local):
        m = mask[:, e : e + 1]
        mine = tok_blk * capacity + rank[:, e : e + 1].astype(jnp.int32)
        hit = jnp.where((slot_ids == mine) & (m > 0.0), 1.0, 0.0)
        comb_ref[:, e * slots : (e + 1) * slots] = (hit * local[:, e : e + 1]).astype(BF16)
        xs_ref[...] = lax.dot_general(
            hit.astype(BF16), x_ref[:, :width], back, preferred_element_type=F32).astype(BF16)
        step = min(hid, 256)
        for n in range(0, hid, step):
            g = jnp.dot(xs_ref[...], gate_ref[e, :, n : n + step], preferred_element_type=F32)
            u = jnp.dot(xs_ref[...], up_ref[e, :, n : n + step], preferred_element_type=F32)
            c = jnp.minimum(g, CLAMP)
            act_ref[e, :, n : n + step] = (
                (jnp.clip(u, -CLAMP, CLAMP) + 1.0) * (c * jax.nn.sigmoid(ALPHA * c))).astype(BF16)


def down_body(groups, act_ref, comb_ref, down_ref, *refs):
    sends, keeps, o_ref = refs[:groups], refs[groups : 2 * groups], refs[2 * groups]
    e_local, slots, _ = act_ref.shape
    width = down_ref.shape[2]
    step = min(width, 512)
    each = keeps[0].shape[0]
    for n in range(0, width, step):
        for e in range(e_local):
            o_ref[e * slots : (e + 1) * slots, :] = jnp.dot(
                act_ref[e], down_ref[e, :, n : n + step], preferred_element_type=F32).astype(BF16)
        y = jnp.dot(comb_ref[...], o_ref[...], preferred_element_type=F32)
        for j in range(groups):
            keeps[j][:, n : n + step] = y[j * each : (j + 1) * each]
            at = (groups + j) * each
            sends[j][:, n : n + step] = y[at : at + each].astype(BF16)


def add_body(a_ref, b_ref, out_ref):
    out_ref[...] = (a_ref[...] + b_ref[...].astype(F32)).astype(out_ref.dtype)


def fold_body(count, z_count, *refs):
    ins, outs = refs[:count], refs[count:]
    rows_each = outs[0].shape[0]
    for k in range(z_count):
        part = slice(k * rows_each, (k + 1) * rows_each)
        total = ins[0][part, :].astype(F32)
        for r in ins[1:]:
            total = total + r[part, :].astype(F32)
        outs[k][...] = total.astype(outs[k].dtype)


def final_body(*refs):
    total = refs[0][...].astype(F32)
    for r in refs[1:-1]:
        total = total + r[...].astype(F32)
    refs[-1][...] = total.astype(BF16)


def per_device(
    tokens, rec_state, conv_state, route_ids, route_weights, first_gain, proj_input, proj_gate,
    conv_taps, decay_logit, block_decay, block_input, rec_gain, proj_out, second_gain,
    expert_gate, expert_up, expert_down,
):
    tp_count = lax.axis_size("tp")
    ep_count = lax.axis_size("ep")
    tp_place = lax.axis_index("tp")
    ep_place = lax.axis_index("ep")
    z_count = tp_count // 2
    lw = proj_input.shape[1]
    own, width = tokens.shape
    seqs = rec_state.shape[0]
    e_local, _, hid = expert_gate.shape
    experts = e_local * ep_count
    top = route_ids.shape[1]
    capacity = max(2, own * top // experts)
    ext = width + LANES

    def z_swap(v, k):
        return lax.ppermute(v, "tp", [(i, ((i // 2) ^ k) * 2 + i % 2) for i in range(tp_count)])

    def core_swap(v):
        return lax.ppermute(v, "tp", [(i, i ^ 1) for i in range(tp_count)])

    def ep_swap(v, j):
        return lax.ppermute(v, "ep", [(i, i ^ j) for i in range(ep_count)])

    mine = [tokens] + [z_swap(tokens, k) for k in range(1, z_count)]
    theirs = [core_swap(v) for v in mine]

    first = tp_place * lw
    taps = lax.dynamic_slice_in_dim(conv_taps, first, lw, 1).astype(F32)
    conv_part = sum(taps[t] * conv_state[:, t].astype(F32) for t in range(conv_state.shape[1]))
    nb = lw // block_decay.shape[1]
    dmat = lax.dynamic_slice_in_dim(block_decay, tp_place * nb, nb, 0)
    imat = lax.dynamic_slice_in_dim(block_input, tp_place * nb, nb, 0)
    rate = -RATE * jax.nn.softplus(-lax.dynamic_slice_in_dim(decay_logit, first, lw, 0))
    rgain = lax.dynamic_slice_in_dim(rec_gain, first, lw, 0).astype(F32)
    ids = lax.dynamic_slice_in_dim(route_ids, tp_place * own, own, 0)
    wdense = jnp.sum(
        jnp.where(ids[:, :, None] == jnp.arange(LANES, dtype=jnp.int32), route_weights[:, :, None], 0.0),
        axis=1).astype(BF16)

    half = seqs // 2
    new_state, branch, keep, send = call(
        functools.partial(recur_body, z_count),
        [((seqs, lw), F32), ((seqs, lw), BF16), ((half, ext), F32), ((half, ext), BF16)],
        [tp_place.reshape(1)] + mine + theirs
        + [first_gain.reshape(1, -1), proj_input, proj_gate, conv_part, taps[-1:], dmat, imat,
           rate.reshape(1, -1), rec_state, rgain.reshape(1, -1), proj_out],
        16, "recur", smem=1)
    got = core_swap(send)
    mixed = call(
        functools.partial(mix_body, z_count),
        [((own, ext), F32)] + [((own, ext), BF16)] * (z_count - 1), [keep, got], 4, "mix")
    parts = [mixed[0]] + [z_swap(mixed[k], k) for k in range(1, z_count)]
    residual, second = call(
        functools.partial(second_body, lw * tp_count, z_count),
        [((own, width), F32), ((own, ext), BF16)],
        [tokens, second_gain.reshape(1, -1), wdense] + parts, 4, "second")

    lines = [second] + [z_swap(second, k) for k in range(1, z_count)]
    (line,) = call(cat_body, [((z_count * own, ext), BF16)], lines, 4, "line")
    mine = [line] + [ep_swap(line, j) for j in range(1, ep_count)]
    theirs = [core_swap(v) for v in mine]
    pieces = mine + theirs
    rows = 2 * ep_count * z_count * own
    slots = 2 * ep_count * z_count * capacity
    act, comb = pl.pallas_call(
        functools.partial(gateup_body, len(pieces), own, capacity),
        out_shape=[jax.ShapeDtypeStruct((e_local, slots, hid), BF16),
                   jax.ShapeDtypeStruct((rows, e_local * slots), BF16)],
        in_specs=[SM] + [VM] * (len(pieces) + 2),
        out_specs=[VM] * 2,
        scratch_shapes=[pltpu.VMEM((rows, ext), BF16), pltpu.VMEM((slots, width), BF16)],
        name="gateup",
        compiler_params=pltpu.CompilerParams(vmem_limit_bytes=max(16, rows // 32) << 20),
        cost_estimate=pl.CostEstimate(flops=10**9, bytes_accessed=10**7, transcendentals=0),
    )(ep_place.reshape(1), *pieces, expert_gate, expert_up)
    each = z_count * own
    outs = pl.pallas_call(
        functools.partial(down_body, ep_count),
        out_shape=[jax.ShapeDtypeStruct((each, width), BF16)] * ep_count
        + [jax.ShapeDtypeStruct((each, width), F32)] * ep_count,
        in_specs=[VM] * 3,
        out_specs=[VM] * (2 * ep_count),
        scratch_shapes=[pltpu.VMEM((e_local * slots, min(width, 512)), BF16)],
        name="down",
        compiler_params=pltpu.CompilerParams(vmem_limit_bytes=max(16, rows // 32) << 20),
        cost_estimate=pl.CostEstimate(flops=10**9, bytes_accessed=10**7, transcendentals=0),
    )(act, comb, expert_down)
    sends, keeps = outs[:ep_count], outs[ep_count:]
    order = list(range(1, ep_count)) + [0]
    got = {j: core_swap(sends[j]) for j in order}
    back = []
    for j in range(1, ep_count):
        (s,) = call(add_body, [((each, width), BF16)], [keeps[j], got[j]], 4, "fold%d" % j)
        back.append(ep_swap(s, j))
    ins = [keeps[0], got[0]] + back
    folded = call(
        functools.partial(fold_body, len(ins), z_count),
        [((own, width), F32)] + [((own, width), BF16)] * (z_count - 1), ins, 8, "foldz")
    last = [folded[0]] + [z_swap(folded[k], k) for k in range(1, z_count)]
    (result,) = call(final_body, [((own, width), BF16)], [residual] + last, 4, "final")
    new_conv = jnp.concatenate([conv_state[:, 1:], branch[:, None, :]], axis=1)
    return (result, new_state, new_conv)


def solution(mesh):
    in_specs = (
        P(("ep", "tp"), None), P("ep", "tp"), P("ep", None, "tp"), P("ep", None),
        P(("ep", "tp"), None), P(), P(None, "tp"), P(None, "tp"), P(), P(), P(), P(), P(),
        P("tp", None), P(), P("ep", None, "tp"), P("ep", None, "tp"), P("ep", "tp", None),
    )
    out_specs = (P(("ep", "tp"), None), P("ep", "tp"), P("ep", None, "tp"))
    return jax.shard_map(
        per_device, mesh=mesh, in_specs=in_specs, out_specs=out_specs, check_vma=False
    )
```

```python
import functools

import jax
import jax.numpy as jnp
from jax import lax
from jax.experimental import pallas as pl
from jax.experimental.pallas import tpu as pltpu
from jax.sharding import PartitionSpec as P

EPS = 1e-06
CLAMP = 7.0
ALPHA = 1.702
RATE = 8.0
LANES = 128
LONG = 3 * 10**10
F32 = jnp.float32
BF16 = jnp.bfloat16


VM = pl.BlockSpec(memory_space=pltpu.VMEM)
SM = pl.BlockSpec(memory_space=pltpu.SMEM)


def call(body, outs, args, limit_mib, name, smem=0, flops=10**8):
    specs = [SM] * smem + [VM] * (len(args) - smem)
    shapes = [jax.ShapeDtypeStruct(s, d) for s, d in outs]
    return pl.pallas_call(
        body,
        out_shape=shapes,
        in_specs=specs,
        out_specs=[VM] * len(outs),
        name=name,
        compiler_params=pltpu.CompilerParams(vmem_limit_bytes=limit_mib << 20),
        cost_estimate=pl.CostEstimate(flops=flops, bytes_accessed=10**6, transcendentals=0),
    )(*args)


def log2(n):
    return n.bit_length() - 1


def split_sum(values):
    high = values.astype(BF16)
    low = (values - high.astype(F32)).astype(BF16)
    lane = lax.broadcasted_iota(jnp.int32, values.shape, 1)
    return jnp.where(lane == 0, high.astype(F32), jnp.where(lane == 1, low.astype(F32), 0.0))


def minus_expm1(u):
    series = -u * (1.0 + u * (0.5 + u * (1.0 / 6.0 + u * (1.0 / 24.0 + u * (1.0 / 120.0)))))
    return jnp.where(u > -0.125, series, 1.0 - jnp.exp(u))


def prep_body(where_ref, ids_ref, wts_ref, dense_ref):
    place = where_ref[0]
    rows_each, rows = dense_ref.shape[0], ids_ref.shape[1]
    along = (((1,), (1,)), ((), ()))
    pick_r = lax.broadcasted_iota(jnp.int32, (rows_each, rows), 0)
    pick_c = lax.broadcasted_iota(jnp.int32, (rows_each, rows), 1)
    pick = jnp.where(pick_c == place * rows_each + pick_r, 1.0, 0.0).astype(BF16)
    ids = lax.dot_general(pick, ids_ref[...].astype(F32).astype(BF16), along, preferred_element_type=F32)
    eye = jnp.where(pick_c == pick_r, 1.0, 0.0).astype(BF16)[:, :rows_each]
    wts = lax.dot_general(eye, wts_ref[...].astype(BF16), along, preferred_element_type=F32)
    lane = lax.broadcasted_iota(jnp.int32, (rows_each, LANES), 1)
    ids = ids.astype(jnp.int32)
    dense = jnp.zeros((rows_each, LANES), F32)
    for t in range(ids.shape[1]):
        dense = dense + jnp.where(lane == ids[:, t : t + 1], wts[:, t : t + 1], 0.0)
    dense_ref[...] = dense.astype(BF16)


def recur_body(z_count, *refs):
    where_ref = refs[0]
    blocks = refs[1 : 1 + 2 * z_count]
    (gain_ref, win_ref, wgate_ref, past_ref, taps_ref, dmat_ref, imat_ref, logit_ref, state_ref,
     rgain_ref, wout_ref, _) = refs[1 + 2 * z_count : 13 + 2 * z_count]
    newstate_ref, newconv_ref, keep_ref, send_ref = refs[13 + 2 * z_count :]
    rows_each, width = blocks[0].shape
    rows = 2 * z_count * rows_each
    lw = win_ref.shape[1]
    place = where_ref[0]
    first = pl.multiple_of(place * lw, lw)
    gain = gain_ref[0:1, :].astype(F32)
    parts = []
    for b in blocks:
        v = b[...].astype(F32)
        scale = lax.rsqrt(jnp.mean(v * v, axis=-1, keepdims=True) + EPS)
        parts.append(v * scale * gain)
    normed = jnp.concatenate(parts, axis=0).astype(BF16)
    bin_rel = jnp.dot(normed, win_ref[...], preferred_element_type=F32).astype(BF16)
    bgate_rel = jnp.dot(normed, wgate_ref[...], preferred_element_type=F32).astype(BF16)
    z_place = lax.shift_right_logical(place, 1)
    core = place & 1
    row = lax.broadcasted_iota(jnp.int32, (rows, rows), 0)
    col = lax.broadcasted_iota(jnp.int32, (rows, rows), 1)
    sh = log2(rows_each)
    blk = lax.shift_right_logical(col, sh)
    kk = blk & (z_count - 1)
    hh = lax.shift_right_logical(blk, log2(z_count))
    target = ((z_place ^ kk) * 2 + (core ^ hh)) * rows_each + (col & (rows_each - 1))
    order = jnp.where(row == target, 1.0, 0.0).astype(BF16)
    branch = jnp.dot(order, bin_rel, preferred_element_type=F32)
    bgate = jnp.dot(order, bgate_rel, preferred_element_type=F32)
    past = past_ref.shape[0]
    taps = taps_ref[:, pl.ds(first, lw)].astype(F32)
    conv = taps[past : past + 1] * branch
    for t in range(past):
        conv = conv + taps[t : t + 1] * past_ref[t].astype(F32)
    for t in range(past - 1):
        newconv_ref[t] = past_ref[t + 1]
    newconv_ref[past - 1] = branch.astype(BF16)
    low = conv.astype(BF16)
    bw = dmat_ref.shape[1]
    nb = lw // bw
    dec = jnp.concatenate(
        [jnp.dot(low[:, n * bw : (n + 1) * bw], dmat_ref[place * nb + n], preferred_element_type=F32)
         for n in range(nb)], axis=1)
    inp = jnp.concatenate(
        [jnp.dot(low[:, n * bw : (n + 1) * bw], imat_ref[place * nb + n], preferred_element_type=F32)
         for n in range(nb)], axis=1)
    rate = -RATE * jax.nn.softplus(-logit_ref[:, pl.ds(first, lw)])
    log_keep = jax.nn.sigmoid(dec) * rate
    new_state = jnp.exp(log_keep) * state_ref[...] + jnp.sqrt(minus_expm1(2.0 * log_keep)) * jax.nn.sigmoid(inp) * conv
    newstate_ref[...] = new_state
    hidden = new_state * jax.nn.gelu(bgate)
    squares = jnp.sum(hidden * hidden, axis=1, keepdims=True)
    sq = split_sum(jnp.broadcast_to(squares, (rows, LANES))).astype(BF16)
    gained = (hidden * rgain_ref[:, pl.ds(first, lw)].astype(F32)).astype(BF16)
    back = (((0,), (0,)), ((), ()))
    g_rel = lax.dot_general(order, gained, back, preferred_element_type=F32).astype(BF16)
    s_rel = lax.dot_general(order, sq, back, preferred_element_type=F32)
    half = rows // 2
    mixed = jnp.dot(g_rel, wout_ref[...], preferred_element_type=F32)
    keep_ref[:, :width] = mixed[:half]
    keep_ref[:, width:] = s_rel[:half]
    send_ref[:, :width] = mixed[half:].astype(BF16)
    send_ref[:, width:] = s_rel[half:].astype(BF16)


def mix_body(z_count, keep_ref, recv_ref, *outs):
    rows_each, ext = outs[0].shape
    width = ext - LANES
    total = keep_ref[:, :width] + recv_ref[:, :width].astype(F32)
    tail = keep_ref[:, width:] + recv_ref[:, width:].astype(F32)
    squares = tail[:, 0:1] + tail[:, 1:2]
    sq = split_sum(jnp.broadcast_to(squares, tail.shape))
    for k in range(z_count):
        part = slice(k * rows_each, (k + 1) * rows_each)
        outs[k][:, :width] = total[part].astype(outs[k].dtype)
        outs[k][:, width:] = sq[part].astype(outs[k].dtype)


def second_body(channels, count, tok_ref, gain_ref, wdense_ref, *refs):
    parts, (res_ref, sec_ref) = refs[:count], refs[count:]
    width = tok_ref.shape[1]
    total = parts[0][:, :width].astype(F32)
    tail = parts[0][:, width:].astype(F32)
    for p in parts[1:]:
        total = total + p[:, :width].astype(F32)
        tail = tail + p[:, width:].astype(F32)
    squares = tail[:, 0:1] + tail[:, 1:2]
    residual = tok_ref[...].astype(F32) + total * lax.rsqrt(squares / channels + EPS)
    res_ref[...] = residual
    scale = lax.rsqrt(jnp.mean(residual * residual, axis=-1, keepdims=True) + EPS)
    sec_ref[:, :width] = (residual * scale * gain_ref[1:2, :].astype(F32)).astype(BF16)
    sec_ref[:, width:] = wdense_ref[...]


def cat_body(*refs):
    out = refs[-1]
    at = 0
    for r in refs[:-1]:
        out[at : at + r.shape[0]] = r[...]
        at += r.shape[0]


def gateup_body(count, rows_each, capacity, place_ref, *refs):
    pieces = refs[:count]
    gate_ref, up_ref, act_ref, comb_ref, x_ref, xs_ref = refs[count:]
    e_local, width, hid = gate_ref.shape
    each = pieces[0].shape[0]
    rows = count * each
    for i, p in enumerate(pieces):
        x_ref[i * each : (i + 1) * each, :] = p[...]
    weights = x_ref[:, width:].astype(F32)
    lane = lax.broadcasted_iota(jnp.int32, (LANES, LANES), 0)
    col = lax.broadcasted_iota(jnp.int32, (LANES, LANES), 1)
    pick = jnp.where((lane == col + place_ref[1] * e_local) & (col < e_local), 1.0, 0.0).astype(BF16)
    local = jnp.dot(x_ref[:, width:], pick, preferred_element_type=F32)
    mask = (local != 0.0).astype(F32)
    r0 = lax.broadcasted_iota(jnp.int32, (rows, rows), 0)
    c0 = lax.broadcasted_iota(jnp.int32, (rows, rows), 1)
    sh = log2(rows_each)
    same = lax.shift_right_logical(r0, sh) == lax.shift_right_logical(c0, sh)
    before = jnp.where(same & (c0 < r0), 1.0, 0.0).astype(BF16)
    rank = jnp.dot(before, mask.astype(BF16), preferred_element_type=F32)
    slots = rows // rows_each * capacity
    tok_blk = lax.shift_right_logical(lax.broadcasted_iota(jnp.int32, (rows, 1), 0), sh)
    slot_ids = lax.broadcasted_iota(jnp.int32, (rows, slots), 1)
    back = (((0,), (0,)), ((), ()))
    for e in range(e_local):
        m = mask[:, e : e + 1]
        mine = tok_blk * capacity + rank[:, e : e + 1].astype(jnp.int32)
        hit = jnp.where((slot_ids == mine) & (m > 0.0), 1.0, 0.0)
        comb_ref[:, e * slots : (e + 1) * slots] = (hit * local[:, e : e + 1]).astype(BF16)
        xs_ref[...] = lax.dot_general(
            hit.astype(BF16), x_ref[:, :width], back, preferred_element_type=F32).astype(BF16)
        step = min(hid, 256)
        for n in range(0, hid, step):
            g = jnp.dot(xs_ref[...], gate_ref[e, :, n : n + step], preferred_element_type=F32)
            u = jnp.dot(xs_ref[...], up_ref[e, :, n : n + step], preferred_element_type=F32)
            c = jnp.minimum(g, CLAMP)
            act_ref[e, :, n : n + step] = (
                (jnp.clip(u, -CLAMP, CLAMP) + 1.0) * (c * jax.nn.sigmoid(ALPHA * c))).astype(BF16)


def down_body(groups, act_ref, comb_ref, down_ref, *refs):
    sends, keeps, o_ref = refs[:groups], refs[groups : 2 * groups], refs[2 * groups]
    e_local, slots, _ = act_ref.shape
    width = down_ref.shape[2]
    step = min(width, 512)
    each = keeps[0].shape[0]
    for n in range(0, width, step):
        for e in range(e_local):
            o_ref[e * slots : (e + 1) * slots, :] = jnp.dot(
                act_ref[e], down_ref[e, :, n : n + step], preferred_element_type=F32).astype(BF16)
        y = jnp.dot(comb_ref[...], o_ref[...], preferred_element_type=F32)
        for j in range(groups):
            keeps[j][:, n : n + step] = y[j * each : (j + 1) * each]
            at = (groups + j) * each
            sends[j][:, n : n + step] = y[at : at + each].astype(BF16)


def add_body(a_ref, b_ref, out_ref):
    out_ref[...] = (a_ref[...] + b_ref[...].astype(F32)).astype(out_ref.dtype)


def fold_body(count, z_count, *refs):
    ins, outs = refs[:count], refs[count:]
    rows_each = outs[0].shape[0]
    for k in range(z_count):
        part = slice(k * rows_each, (k + 1) * rows_each)
        total = ins[0][part, :].astype(F32)
        for r in ins[1:]:
            total = total + r[part, :].astype(F32)
        outs[k][...] = total.astype(outs[k].dtype)


def final_body(*refs):
    total = refs[0][...].astype(F32)
    for r in refs[1:-1]:
        total = total + r[...].astype(F32)
    refs[-1][...] = total.astype(BF16)


def per_device(
    tokens, rec_state, conv_state, route_ids, route_weights, first_gain, proj_input, proj_gate,
    conv_taps, decay_logit, block_decay, block_input, rec_gain, proj_out, second_gain,
    expert_gate, expert_up, expert_down,
):
    tp_count = lax.axis_size("tp")
    ep_count = lax.axis_size("ep")
    tp_place = lax.axis_index("tp")
    ep_place = lax.axis_index("ep")
    z_count = tp_count // 2
    lw = proj_input.shape[1]
    own, width = tokens.shape
    seqs = rec_state.shape[0]
    e_local, _, hid = expert_gate.shape
    experts = e_local * ep_count
    top = route_ids.shape[1]
    capacity = max(2, own * top // experts)
    ext = width + LANES

    def z_swap(v, k):
        return lax.ppermute(v, "tp", [(i, ((i // 2) ^ k) * 2 + i % 2) for i in range(tp_count)])

    def core_swap(v):
        return lax.ppermute(v, "tp", [(i, i ^ 1) for i in range(tp_count)])

    def ep_swap(v, j):
        return lax.ppermute(v, "ep", [(i, i ^ j) for i in range(ep_count)])

    where = jnp.stack([tp_place, ep_place]).astype(jnp.int32)
    where, start = lax.optimization_barrier((where, tokens))
    mine = [start] + [z_swap(start, k) for k in range(1, z_count)]
    theirs = [core_swap(v) for v in mine]

    (wdense,) = call(
        prep_body, [((own, LANES), BF16)],
        [where, jnp.transpose(route_ids), jnp.transpose(route_weights)], 1, "prep", smem=1, flops=LONG)
    gains = jnp.stack([first_gain, second_gain])
    past = jnp.transpose(conv_state, (1, 0, 2))
    half = seqs // 2
    new_state, new_conv, keep, send = call(
        functools.partial(recur_body, z_count),
        [((seqs, lw), F32), (past.shape, BF16), ((half, ext), F32), ((half, ext), BF16)],
        [where] + mine + theirs
        + [gains, proj_input, proj_gate, past, conv_taps, block_decay, block_input,
           decay_logit.reshape(1, -1), rec_state, rec_gain.reshape(1, -1), proj_out, wdense],
        8, "recur", smem=1)
    got = core_swap(send)
    mixed = call(
        functools.partial(mix_body, z_count),
        [((own, ext), F32)] + [((own, ext), BF16)] * (z_count - 1), [keep, got], 4, "mix")
    parts = [mixed[0]] + [z_swap(mixed[k], k) for k in range(1, z_count)]
    residual, second = call(
        functools.partial(second_body, lw * tp_count, z_count),
        [((own, width), F32), ((own, ext), BF16)],
        [tokens, gains, wdense] + parts, 4, "second")

    lines = [second] + [z_swap(second, k) for k in range(1, z_count)]
    (line,) = call(cat_body, [((z_count * own, ext), BF16)], lines, 4, "line", flops=LONG)
    mine = [line] + [ep_swap(line, j) for j in range(1, ep_count)]
    theirs = [core_swap(v) for v in mine]
    pieces = mine + theirs
    rows = 2 * ep_count * z_count * own
    slots = 2 * ep_count * z_count * capacity
    act, comb = pl.pallas_call(
        functools.partial(gateup_body, len(pieces), own, capacity),
        out_shape=[jax.ShapeDtypeStruct((e_local, slots, hid), BF16),
                   jax.ShapeDtypeStruct((rows, e_local * slots), BF16)],
        in_specs=[SM] + [VM] * (len(pieces) + 2),
        out_specs=[VM] * 2,
        scratch_shapes=[pltpu.VMEM((rows, ext), BF16), pltpu.VMEM((slots, width), BF16)],
        name="gateup",
        compiler_params=pltpu.CompilerParams(vmem_limit_bytes=max(10, rows // 32) << 20),
        cost_estimate=pl.CostEstimate(flops=10**9, bytes_accessed=10**7, transcendentals=0),
    )(where, *pieces, expert_gate, expert_up)
    each = z_count * own
    outs = pl.pallas_call(
        functools.partial(down_body, ep_count),
        out_shape=[jax.ShapeDtypeStruct((each, width), BF16)] * ep_count
        + [jax.ShapeDtypeStruct((each, width), F32)] * ep_count,
        in_specs=[VM] * 3,
        out_specs=[VM] * (2 * ep_count),
        scratch_shapes=[pltpu.VMEM((e_local * slots, min(width, 512)), BF16)],
        name="down",
        compiler_params=pltpu.CompilerParams(vmem_limit_bytes=max(10, rows // 32) << 20),
        cost_estimate=pl.CostEstimate(flops=10**9, bytes_accessed=10**7, transcendentals=0),
    )(act, comb, expert_down)
    sends, keeps = outs[:ep_count], outs[ep_count:]
    order = list(range(1, ep_count)) + [0]
    got = {j: core_swap(sends[j]) for j in order}
    back = []
    for j in range(1, ep_count):
        (s,) = call(add_body, [((each, width), BF16)], [keeps[j], got[j]], 4, "fold%d" % j)
        back.append(ep_swap(s, j))
    ins = [keeps[0], got[0]] + back
    folded = call(
        functools.partial(fold_body, len(ins), z_count),
        [((own, width), F32)] + [((own, width), BF16)] * (z_count - 1), ins, 8, "foldz")
    last = [folded[0]] + [z_swap(folded[k], k) for k in range(1, z_count)]
    (result,) = call(final_body, [((own, width), BF16)], [residual] + last, 4, "final")
    return (result, new_state, jnp.transpose(new_conv, (1, 0, 2)))


def solution(mesh):
    in_specs = (
        P(("ep", "tp"), None), P("ep", "tp"), P("ep", None, "tp"), P("ep", None),
        P(("ep", "tp"), None), P(), P(None, "tp"), P(None, "tp"), P(), P(), P(), P(), P(),
        P("tp", None), P(), P("ep", None, "tp"), P("ep", None, "tp"), P("ep", "tp", None),
    )
    out_specs = (P(("ep", "tp"), None), P("ep", "tp"), P("ep", None, "tp"))
    return jax.shard_map(
        per_device, mesh=mesh, in_specs=in_specs, out_specs=out_specs, check_vma=False
    )
```

```python
import functools

import jax
import jax.numpy as jnp
from jax import lax
from jax.experimental import pallas as pl
from jax.experimental.pallas import tpu as pltpu
from jax.sharding import PartitionSpec as P


EPS = 1e-06
CLAMP = 7.0
ALPHA = 1.702
RATE = 8.0
LANES = 128
LONG = 3 * 10**10
F32 = jnp.float32
BF16 = jnp.bfloat16


VM = pl.BlockSpec(memory_space=pltpu.VMEM)
SM = pl.BlockSpec(memory_space=pltpu.SMEM)


def call(body, outs, args, limit_mib, smem=0, flops=10**8):
    specs = [SM] * smem + [VM] * (len(args) - smem)
    shapes = [jax.ShapeDtypeStruct(s, d) for s, d in outs]
    return pl.pallas_call(
        body,
        out_shape=shapes,
        in_specs=specs,
        out_specs=[VM] * len(outs),
        compiler_params=pltpu.CompilerParams(vmem_limit_bytes=limit_mib << 20),
        cost_estimate=pl.CostEstimate(flops=flops, bytes_accessed=10**6, transcendentals=0),
    )(*args)


def log2(n):
    return n.bit_length() - 1


def split_sum(values):
    high = values.astype(BF16)
    low = (values - high.astype(F32)).astype(BF16)
    lane = lax.broadcasted_iota(jnp.int32, values.shape, 1)
    return jnp.where(lane == 0, high.astype(F32), jnp.where(lane == 1, low.astype(F32), 0.0))


def minus_expm1(u):
    series = -u * (1.0 + u * (0.5 + u * (1.0 / 6.0 + u * (1.0 / 24.0 + u * (1.0 / 120.0)))))
    return jnp.where(u > -0.125, series, 1.0 - jnp.exp(u))


def prep_body(where_ref, ids_ref, wts_ref, dense_ref):
    place = where_ref[0]
    rows_each, rows = dense_ref.shape[0], ids_ref.shape[1]
    along = (((1,), (1,)), ((), ()))
    pick_r = lax.broadcasted_iota(jnp.int32, (rows_each, rows), 0)
    pick_c = lax.broadcasted_iota(jnp.int32, (rows_each, rows), 1)
    pick = jnp.where(pick_c == place * rows_each + pick_r, 1.0, 0.0).astype(BF16)
    ids = lax.dot_general(pick, ids_ref[...].astype(F32).astype(BF16), along, preferred_element_type=F32)
    eye = jnp.where(pick_c == pick_r, 1.0, 0.0).astype(BF16)[:, :rows_each]
    wts = lax.dot_general(eye, wts_ref[...].astype(BF16), along, preferred_element_type=F32)
    lane = lax.broadcasted_iota(jnp.int32, (rows_each, LANES), 1)
    ids = ids.astype(jnp.int32)
    dense = jnp.zeros((rows_each, LANES), F32)
    for t in range(ids.shape[1]):
        dense = dense + jnp.where(lane == ids[:, t : t + 1], wts[:, t : t + 1], 0.0)
    dense_ref[...] = dense.astype(BF16)


def recur_body(z_count, *refs):
    where_ref = refs[0]
    blocks = refs[1 : 1 + 2 * z_count]
    (gain_ref, win_ref, wgate_ref, past_ref, taps_ref, dmat_ref, imat_ref, logit_ref, state_ref,
     rgain_ref, wout_ref, _) = refs[1 + 2 * z_count : 13 + 2 * z_count]
    newstate_ref, newconv_ref, keep_ref, send_ref = refs[13 + 2 * z_count :]
    rows_each, width = blocks[0].shape
    rows = 2 * z_count * rows_each
    lw = win_ref.shape[1]
    place = where_ref[0]
    first = pl.multiple_of(place * lw, lw)
    gain = gain_ref[0:1, :].astype(F32)
    parts = []
    for b in blocks:
        v = b[...].astype(F32)
        scale = lax.rsqrt(jnp.mean(v * v, axis=-1, keepdims=True) + EPS)
        parts.append(v * scale * gain)
    normed = jnp.concatenate(parts, axis=0).astype(BF16)
    bin_rel = jnp.dot(normed, win_ref[...], preferred_element_type=F32).astype(BF16)
    bgate_rel = jnp.dot(normed, wgate_ref[...], preferred_element_type=F32).astype(BF16)
    z_place = lax.shift_right_logical(place, 1)
    core = place & 1
    row = lax.broadcasted_iota(jnp.int32, (rows, rows), 0)
    col = lax.broadcasted_iota(jnp.int32, (rows, rows), 1)
    sh = log2(rows_each)
    blk = lax.shift_right_logical(col, sh)
    kk = blk & (z_count - 1)
    hh = lax.shift_right_logical(blk, log2(z_count))
    target = ((z_place ^ kk) * 2 + (core ^ hh)) * rows_each + (col & (rows_each - 1))
    order = jnp.where(row == target, 1.0, 0.0).astype(BF16)
    branch = jnp.dot(order, bin_rel, preferred_element_type=F32)
    bgate = jnp.dot(order, bgate_rel, preferred_element_type=F32)
    past = past_ref.shape[0]
    taps = taps_ref[:, pl.ds(first, lw)].astype(F32)
    conv = taps[past : past + 1] * branch
    for t in range(past):
        conv = conv + taps[t : t + 1] * past_ref[t].astype(F32)
    for t in range(past - 1):
        newconv_ref[t] = past_ref[t + 1]
    newconv_ref[past - 1] = branch.astype(BF16)
    low = conv.astype(BF16)
    bw = dmat_ref.shape[1]
    nb = lw // bw
    dec = jnp.concatenate(
        [jnp.dot(low[:, n * bw : (n + 1) * bw], dmat_ref[place * nb + n], preferred_element_type=F32)
         for n in range(nb)], axis=1)
    inp = jnp.concatenate(
        [jnp.dot(low[:, n * bw : (n + 1) * bw], imat_ref[place * nb + n], preferred_element_type=F32)
         for n in range(nb)], axis=1)
    rate = -RATE * jax.nn.softplus(-logit_ref[:, pl.ds(first, lw)])
    log_keep = jax.nn.sigmoid(dec) * rate
    new_state = jnp.exp(log_keep) * state_ref[...] + jnp.sqrt(minus_expm1(2.0 * log_keep)) * jax.nn.sigmoid(inp) * conv
    newstate_ref[...] = new_state
    hidden = new_state * jax.nn.gelu(bgate)
    squares = jnp.sum(hidden * hidden, axis=1, keepdims=True)
    sq = split_sum(jnp.broadcast_to(squares, (rows, LANES))).astype(BF16)
    gained = (hidden * rgain_ref[:, pl.ds(first, lw)].astype(F32)).astype(BF16)
    back = (((0,), (0,)), ((), ()))
    g_rel = lax.dot_general(order, gained, back, preferred_element_type=F32).astype(BF16)
    s_rel = lax.dot_general(order, sq, back, preferred_element_type=F32)
    half = rows // 2
    mixed = jnp.dot(g_rel, wout_ref[...], preferred_element_type=F32)
    keep_ref[:, :width] = mixed[:half]
    keep_ref[:, width:] = s_rel[:half]
    send_ref[:, :width] = mixed[half:].astype(BF16)
    send_ref[:, width:] = s_rel[half:].astype(BF16)


def mix_body(z_count, keep_ref, recv_ref, *outs):
    rows_each, ext = outs[0].shape
    width = ext - LANES
    total = keep_ref[:, :width] + recv_ref[:, :width].astype(F32)
    tail = keep_ref[:, width:] + recv_ref[:, width:].astype(F32)
    squares = tail[:, 0:1] + tail[:, 1:2]
    sq = split_sum(jnp.broadcast_to(squares, tail.shape))
    for k in range(z_count):
        part = slice(k * rows_each, (k + 1) * rows_each)
        outs[k][:, :width] = total[part].astype(outs[k].dtype)
        outs[k][:, width:] = sq[part].astype(outs[k].dtype)


def second_body(channels, count, tok_ref, gain_ref, wdense_ref, *refs):
    parts, (res_ref, sec_ref) = refs[:count], refs[count:]
    width = tok_ref.shape[1]
    total = parts[0][:, :width].astype(F32)
    tail = parts[0][:, width:].astype(F32)
    for p in parts[1:]:
        total = total + p[:, :width].astype(F32)
        tail = tail + p[:, width:].astype(F32)
    squares = tail[:, 0:1] + tail[:, 1:2]
    residual = tok_ref[...].astype(F32) + total * lax.rsqrt(squares / channels + EPS)
    res_ref[...] = residual
    scale = lax.rsqrt(jnp.mean(residual * residual, axis=-1, keepdims=True) + EPS)
    sec_ref[:, :width] = (residual * scale * gain_ref[1:2, :].astype(F32)).astype(BF16)
    sec_ref[:, width:] = wdense_ref[...]


def cat_body(*refs):
    out = refs[-1]
    at = 0
    for r in refs[:-1]:
        out[at : at + r.shape[0]] = r[...]
        at += r.shape[0]


def gateup_body(count, rows_each, capacity, where_ref, *refs):
    pieces = refs[:count]
    gate_ref, up_ref, act_ref, comb_ref, x_ref, xs_ref = refs[count:]
    e_local, width, _ = gate_ref.shape
    each = pieces[0].shape[0]
    rows = count * each
    tags = []
    for i, p in enumerate(pieces):
        x_ref[i * each : (i + 1) * each, :] = p[:, :width]
        tags.append(p[:, width:])
    tags = jnp.concatenate(tags, axis=0)
    slots = rows // rows_each * capacity
    wide = e_local * slots
    first = where_ref[1] * e_local
    lane = lax.broadcasted_iota(jnp.int32, (LANES, wide), 0)
    col = lax.broadcasted_iota(jnp.int32, (LANES, wide), 1)
    pick = jnp.where(lane == lax.shift_right_logical(col, log2(slots)) + first, 1.0, 0.0).astype(BF16)
    weight = jnp.dot(tags, pick, preferred_element_type=F32)
    r0 = lax.broadcasted_iota(jnp.int32, (rows, rows), 0)
    c0 = lax.broadcasted_iota(jnp.int32, (rows, rows), 1)
    sh = log2(rows_each)
    same = lax.shift_right_logical(r0, sh) == lax.shift_right_logical(c0, sh)
    before = jnp.where(same & (c0 < r0), 1.0, 0.0).astype(BF16)
    mask = jnp.where(weight != 0.0, 1.0, 0.0).astype(BF16)
    rank = jnp.dot(before, mask, preferred_element_type=F32).astype(jnp.int32)
    blk = lax.shift_right_logical(lax.broadcasted_iota(jnp.int32, (rows, wide), 0), sh)
    slot = lax.broadcasted_iota(jnp.int32, (rows, wide), 1) & (slots - 1)
    hit = slot == blk * capacity + rank
    comb_ref[...] = jnp.where(hit, weight, 0.0).astype(BF16)
    chosen = jnp.where(hit & (weight != 0.0), 1.0, 0.0).astype(BF16)
    back = (((0,), (0,)), ((), ()))
    step = min(width, 1024)
    for n in range(0, width, step):
        xs_ref[:, n : n + step] = lax.dot_general(
            chosen, x_ref[:, n : n + step], back, preferred_element_type=F32).astype(BF16)
    for e in range(e_local):
        xs = xs_ref[e * slots : (e + 1) * slots, :]
        g = jnp.dot(xs, gate_ref[e], preferred_element_type=F32)
        u = jnp.dot(xs, up_ref[e], preferred_element_type=F32)
        c = jnp.minimum(g, CLAMP)
        act_ref[e] = ((jnp.clip(u, -CLAMP, CLAMP) + 1.0) * (c * jax.nn.sigmoid(ALPHA * c))).astype(BF16)


def down_body(act_ref, comb_ref, down_ref, *refs):
    outs, o_ref = refs[:-1], refs[-1]
    sends, keeps = outs[: len(outs) // 2], outs[len(outs) // 2 :]
    e_local, slots, _ = act_ref.shape
    width = down_ref.shape[2]
    step = min(width, 1024)
    for e in range(e_local):
        for n in range(0, width, step):
            o_ref[e * slots : (e + 1) * slots, n : n + step] = jnp.dot(
                act_ref[e], down_ref[e, :, n : n + step], preferred_element_type=F32).astype(BF16)
    for n in range(0, width, step):
        y = jnp.dot(comb_ref[...], o_ref[:, n : n + step], preferred_element_type=F32)
        at = 0
        for k in keeps:
            k[:, n : n + step] = y[at : at + k.shape[0]]
            at += k.shape[0]
        for k in sends:
            k[:, n : n + step] = y[at : at + k.shape[0]].astype(BF16)
            at += k.shape[0]


def fold_body(cuts, starts, *refs):
    ins, outs = refs[: len(starts)], refs[len(starts) :]
    for (at, size), out in zip(cuts, outs):
        total = None
        for r, s in zip(ins, starts):
            v = r[s + at : s + at + size, :].astype(F32)
            total = v if total is None else total + v
        out[...] = total.astype(out.dtype)


def final_body(*refs):
    total = refs[0][...].astype(F32)
    for r in refs[1:-1]:
        total = total + r[...].astype(F32)
    refs[-1][...] = total.astype(BF16)


def per_device(
    tokens, rec_state, conv_state, route_ids, route_weights, first_gain, proj_input, proj_gate,
    conv_taps, decay_logit, block_decay, block_input, rec_gain, proj_out, second_gain,
    expert_gate, expert_up, expert_down,
):
    tp_count = lax.axis_size("tp")
    ep_count = lax.axis_size("ep")
    tp_place = lax.axis_index("tp")
    ep_place = lax.axis_index("ep")
    z_count = tp_count // 2
    lw = proj_input.shape[1]
    own, width = tokens.shape
    seqs = rec_state.shape[0]
    e_local, _, hid = expert_gate.shape
    experts = e_local * ep_count
    top = route_ids.shape[1]
    capacity = max(2, own * top // experts)
    ext = width + LANES

    def z_swap(v, k):
        return lax.ppermute(v, "tp", [(i, ((i // 2) ^ k) * 2 + i % 2) for i in range(tp_count)])

    def core_swap(v):
        return lax.ppermute(v, "tp", [(i, i ^ 1) for i in range(tp_count)])

    where = jnp.stack([tp_place, ep_place]).astype(jnp.int32)
    where, start = lax.optimization_barrier((where, tokens))
    mine = [start] + [z_swap(start, k) for k in range(1, z_count)]
    theirs = [core_swap(v) for v in mine]

    (wdense,) = call(
        prep_body, [((own, LANES), BF16)],
        [where, jnp.transpose(route_ids), jnp.transpose(route_weights)], 1, smem=1, flops=LONG)
    gains = jnp.stack([first_gain, second_gain])
    past = jnp.transpose(conv_state, (1, 0, 2))
    half = seqs // 2
    new_state, new_conv, keep, send = call(
        functools.partial(recur_body, z_count),
        [((seqs, lw), F32), (past.shape, BF16), ((half, ext), F32), ((half, ext), BF16)],
        [where] + mine + theirs
        + [gains, proj_input, proj_gate, past, conv_taps, block_decay, block_input,
           decay_logit.reshape(1, -1), rec_state, rec_gain.reshape(1, -1), proj_out, wdense],
        8, smem=1)
    got = core_swap(send)
    mixed = call(
        functools.partial(mix_body, z_count),
        [((own, ext), F32)] + [((own, ext), BF16)] * (z_count - 1), [keep, got], 4)
    parts = [mixed[0]] + [z_swap(mixed[k], k) for k in range(1, z_count)]
    residual, second = call(
        functools.partial(second_body, lw * tp_count, z_count),
        [((own, width), F32), ((own, ext), BF16)],
        [tokens, gains, wdense] + parts, 4, flops=LONG)

    side = 1 << (log2(ep_count) // 2)
    square = side * side == ep_count

    def pair_swap(v, a, which):
        def go(i):
            e, t = i // tp_count, i % tp_count
            low = (which == 0) if (t % 2 == 0 or not square) else (which == 1)
            return (e ^ a if low else e ^ (a * side)) * tp_count + t

        return lax.ppermute(v, ("ep", "tp"), [(i, go(i)) for i in range(ep_count * tp_count)])

    n_first, n_second = range(1, side), range(1, ep_count // side)
    lines = [second] + [z_swap(second, k) for k in range(1, z_count)]
    near = z_count // 2
    pieces = []
    for group in (lines[:near], lines[near:]):
        (line,) = call(cat_body, [((near * own, ext), BF16)], group, 4, flops=10**8)
        ones = [pair_swap(line, a, 0) for a in n_first]
        twos = [pair_swap(line, b, 1) for b in n_second]
        threes = [pair_swap(v, b, 1) for v in ones for b in n_second]
        pieces.append([line] + ones + twos + threes)
    flat = pieces[1] + pieces[0]
    flat = flat + [core_swap(v) for v in flat]
    rows = 2 * ep_count * z_count * own
    slots = 2 * ep_count * z_count * capacity
    act, comb = pl.pallas_call(
        functools.partial(gateup_body, len(flat), own, capacity),
        out_shape=[jax.ShapeDtypeStruct((e_local, slots, hid), BF16),
                   jax.ShapeDtypeStruct((rows, e_local * slots), BF16)],
        in_specs=[SM] + [VM] * (len(flat) + 2),
        out_specs=[VM] * 2,
        scratch_shapes=[pltpu.VMEM((rows, width), BF16), pltpu.VMEM((e_local * slots, width), BF16)],
        name="gateup",
        compiler_params=pltpu.CompilerParams(vmem_limit_bytes=max(10, rows // 26) << 20),
        cost_estimate=pl.CostEstimate(flops=10**9, bytes_accessed=10**7, transcendentals=0),
    )(where, *flat, expert_gate, expert_up)
    each = near * own
    n_rest = 1 + len(n_first) + len(n_second)
    n_three = len(n_first) * len(n_second)
    shapes = [n_rest * each, n_three * each] * 2
    outs = pl.pallas_call(
        down_body,
        out_shape=[jax.ShapeDtypeStruct((r, width), BF16) for r in shapes]
        + [jax.ShapeDtypeStruct((r, width), F32) for r in shapes],
        in_specs=[VM] * 3,
        out_specs=[VM] * 8,
        scratch_shapes=[pltpu.VMEM((e_local * slots, width), BF16)],
        name="down",
        compiler_params=pltpu.CompilerParams(vmem_limit_bytes=max(10, rows // 26) << 20),
        cost_estimate=pl.CostEstimate(flops=10**9, bytes_accessed=10**7, transcendentals=0),
    )(act, comb, expert_down)
    sends, keeps = outs[:4], outs[4:]
    got = {i: core_swap(sends[i]) for i in (1, 0, 3, 2)}
    blocks = []
    for h in (0, 1):
        rest, three = 2 * h, 2 * h + 1
        t_out = call(
            functools.partial(fold_body, [(i * each, each) for i in range(n_three)], [0, 0]),
            [((each, width), BF16)] * n_three, [keeps[three], got[three]], 4)
        t_back = [pair_swap(t_out[i], n_second[i % len(n_second)], 1) for i in range(n_three)]
        two_at = (1 + len(n_first)) * each
        two_out = call(
            functools.partial(fold_body, [(i * each, each) for i in range(len(n_second))], [two_at, two_at]),
            [((each, width), BF16)] * len(n_second), [keeps[rest], got[rest]], 4)
        two_back = [pair_swap(two_out[i], b, 1) for i, b in enumerate(n_second)]
        one_back = []
        for i, a in enumerate(n_first):
            extra = t_back[i * len(n_second) : (i + 1) * len(n_second)]
            at = (1 + i) * each
            (one,) = call(
                functools.partial(fold_body, [(0, each)], [at, at] + [0] * len(extra)),
                [((each, width), BF16)], [keeps[rest], got[rest]] + extra, 4)
            one_back.append(pair_swap(one, a, 0))
        ins = [keeps[rest], got[rest]] + one_back + two_back
        blocks.append(call(
            functools.partial(fold_body, [(k * own, own) for k in range(near)], [0] * len(ins)),
            [((own, width), F32 if (h == 1 and k == 0) else BF16) for k in range(near)], ins, 4))
    folded = list(blocks[1]) + list(blocks[0])
    last = [folded[0]] + [z_swap(folded[k], k) for k in range(1, z_count)]
    (result,) = call(final_body, [((own, width), BF16)], [residual] + last, 4)
    return (result, new_state, jnp.transpose(new_conv, (1, 0, 2)))


def solution(mesh):
    in_specs = (
        P(("ep", "tp"), None), P("ep", "tp"), P("ep", None, "tp"), P("ep", None),
        P(("ep", "tp"), None), P(), P(None, "tp"), P(None, "tp"), P(), P(), P(), P(), P(),
        P("tp", None), P(), P("ep", None, "tp"), P("ep", None, "tp"), P("ep", "tp", None),
    )
    out_specs = (P(("ep", "tp"), None), P("ep", "tp"), P("ep", None, "tp"))

    return jax.shard_map(per_device, mesh=mesh, in_specs=in_specs, out_specs=out_specs, check_vma=False)
```
